512 devices in a mesh: grp: 2 (over y), ep: 32 (over z, core), tp: 8 (over x).
Axes of the slice: x: 8, y: 2, z: 16, core: 2. Of those that a mesh axis runs over, the one named last changes fastest.
The devices are a block of a 8x8x16 slice.
Arguments:
- tokens: bfloat16 [16384, 2048], P(('grp', 'ep')), parts along dimension 0, may hold values from -6 to 6
- in_gain: bfloat16 [2048], replicated, may hold values from 0.099609375 to 1.8984375
- expert_ids: int32 [16384, 2], P(('grp', 'ep')), parts along dimension 0, may hold values from 0 to 31, all different within a row; in each aligned block of 256 rows (0 to 255, 256 to 511, ...) at most 32 rows name the same one
- route_weights: float32 [16384, 2], P(('grp', 'ep')), parts along dimension 0, may hold values from 0.1 to 1
- gate_weight: bfloat16 [32, 2048, 2048], P('ep', None, 'tp'), may hold values from -0.375 to 0.375
- up_weight: bfloat16 [32, 2048, 2048], P('ep', None, 'tp'), may hold values from -0.375 to 0.375
- down_weight: bfloat16 [32, 2048, 2048], P('ep', 'tp')
- out_gain: bfloat16 [2048], P('tp'), may hold values from 0.099609375 to 1.8984375
Outputs:
- normed_out: bfloat16 [16384, 2048], P(('grp', 'ep'), 'tp'), parts along dimension 0
The draws below stay inside these ranges and needn't reach their ends.
There are 2 independent parts, one for each index of `grp`. The reference program is written for one: setup_inputs(seed, part) draws one part's arguments, and reference() takes and returns one part's arrays. A program takes and returns all parts, laid end to end along the dimension named above; an argument that names none is the same for every part. Nothing has to cross between parts.
Inputs may be any that keep to these rules, and one draw needn't show every extreme that they name: `expert_ids`: each row names 2 different experts. Among the 256 rows of one index of ep, no expert is named more than 32 times, a bound that some block reaches.
All inputs are finite; a program needn't handle non-finite values.
Results may differ from the reference program's by a relative error of at most 0.015.
Values may be sent and summed in bfloat16 or wider, within the bound.
A program may use at most 64 MiB of HBM per device.

```python
import math
import jax
import jax.numpy as jnp
import numpy as np
from jax import lax

D = 2048
FF = 2048
TOP_K = 2
TOK_DEV = 256
EXPERTS = 32
TOKENS = 8192
CAP = 32
N_EP = 32
N_TP = 8


def draw_down_weight(key, part):
    column = jnp.arange(D, dtype=jnp.float32) / D
    entries = jax.random.normal(key, (EXPERTS, FF, D), jnp.float32)
    scales = jnp.exp(jnp.log(4.0) * column)
    return (entries * scales[None, None, :] * FF ** (-0.5)).astype(jnp.bfloat16)


def level_of(stream_key, dims, shards, least, high):
    def one(position, shards_of):
        heights = jax.random.uniform(jax.random.fold_in(jax.random.fold_in(stream_key, 6), position), (shards_of,), jnp.float32, least / len(shards), high / len(shards))
        return jnp.repeat(jnp.exp(heights), dims[position] // shards_of).reshape((-1,) + (1,) * (len(dims) - position - 1))

    loudness = one(*shards[0])
    for cut in shards[1:]:
        loudness = loudness * one(*cut)
    return loudness


def routed_block(rng, own, number, rows, number_of, top, bound, slope):
    sequence = jax.random.permutation(rng, number_of)
    heavy_load, common = shares(number_of, rows * top, bound, slope, True), shares(number_of, rows * top, bound, slope, False)
    places = jnp.arange(number_of)

    def named(lengths, offset_by):
        used = int((lengths > 0).sum())
        fixed = max(1, used // 4)
        moved = fixed + (places - fixed + offset_by * (used - fixed)) % max(1, number_of - fixed)
        return jnp.zeros((number_of,), jnp.int32).at[sequence[jnp.where(places < fixed, places, moved)]].set(jnp.asarray(lengths, jnp.int32))

    lengths = jnp.where(number % 4 == 0, named(heavy_load, number // 4), named(common, number - number // 4 - 1))
    mixed = jax.random.permutation(jax.random.fold_in(own, 3), number_of)
    giver, taker = mixed[0:number_of // 2 * 2:2], mixed[1:number_of // 2 * 2:2]
    margin = jnp.minimum(lengths[giver] - 1, bound - lengths[taker]) // 2
    margin = jnp.where((giver == sequence[0]) | (taker == sequence[0]) | (lengths[taker] == 0), 0, jnp.maximum(margin, 0))
    moved = jax.random.randint(jax.random.fold_in(own, 4), (number_of // 2,), 0, 1 << 20) % (margin + 1)
    lengths = lengths.at[giver].add(-moved).at[taker].add(moved)
    items = jnp.searchsorted(jnp.cumsum(lengths), jnp.arange(rows * top), side="right").astype(jnp.int32)
    listing = items.reshape(top, rows).T
    listing = listing[jax.random.permutation(jax.random.fold_in(own, 1), rows)]
    offset_by = jax.random.randint(jax.random.fold_in(own, 2), (rows, 1), 0, top)
    return jnp.take_along_axis(listing, (jnp.arange(top)[None, :] + offset_by) % top, axis=1)


def shares(number_of, total, limit, lean, full):
    weights = [(1 << 20) // math.isqrt(grade ** lean) + 1 for grade in range(1, number_of + 1)]
    largest = limit if full else min(limit, max(-(-total // number_of), total * weights[0] // sum(weights)))
    least = 1 if total - largest >= number_of - 1 else 0
    given, surplus = [largest] + [least] * (number_of - 1), total - largest - least * (number_of - 1)
    while surplus > 0:
        free = [i for i in range(1, number_of) if given[i] < largest] or [i for i in range(1, number_of) if given[i] < limit]
        mass, left = sum([weights[i] for i in free]), surplus
        for i in free:
            addition = min(limit - given[i], max(1, left * weights[i] // mass), surplus)
            given[i] = given[i] + addition
            surplus = surplus - addition
    return np.array(given)


def centred(key, extent, spread, limit, cuts=(), kind=jnp.bfloat16):
    loudness = level_of(key, extent, cuts, -0.22, 0.18) if cuts else 1.0
    array = jax.random.normal(key, extent, jnp.float32) * spread * loudness
    return jnp.minimum(jnp.maximum(array, -limit), limit).astype(kind)


def setup_inputs(seed: int = 0, part: int = 0) -> dict:
    keys = jax.random.split(jax.random.key(seed), 9)
    part_splits = jax.random.split(jax.random.fold_in(keys[8], part), 9)
    tokens = centred(part_splits[0], (TOKENS, D), 1.0, 6.0, ((0, 32),))
    in_gain = jnp.clip(1.0 + 0.18 * jax.random.normal(keys[1], (D,), jnp.float32), 0.099609375, 1.8984375).astype(jnp.bfloat16)
    expert_ids_keys = jax.random.split(jax.random.fold_in(part_splits[2], 1), TOKENS // TOK_DEV)
    expert_ids_turns = jax.random.permutation(jax.random.fold_in(part_splits[2], 3), TOKENS // TOK_DEV)
    expert_ids = jax.vmap(lambda own, number: routed_block(jax.random.fold_in(part_splits[2], 2), own, number, TOK_DEV, EXPERTS, TOP_K, CAP, 2))(expert_ids_keys, expert_ids_turns).reshape((TOKENS, TOP_K))
    route_weights = jnp.clip(jnp.exp(math.log(1.0) - 2.3025851 * jax.random.uniform(part_splits[3], (TOKENS, TOP_K), jnp.float32) ** level_of(part_splits[3], (TOKENS, TOP_K), ((0, 32),), -0.2, 0.2)), 0.1, 1.0)
    gate_weight = centred(keys[4], (EXPERTS, D, FF), (D // 8) ** -0.5, 0.375, ((0, 32), (2, 8)))
    up_weight = centred(keys[5], (EXPERTS, D, FF), (D // 8) ** -0.5, 0.375, ((0, 32), (2, 8)))
    down_weight = draw_down_weight(jax.random.fold_in(keys[8], 71), part)
    out_gain = jnp.clip(1.0 + 0.18 * jax.random.normal(keys[7], (D,), jnp.float32), 0.099609375, 1.8984375).astype(jnp.bfloat16)
    return dict(tokens=tokens, in_gain=in_gain, expert_ids=expert_ids, route_weights=route_weights, gate_weight=gate_weight, up_weight=up_weight, down_weight=down_weight, out_gain=out_gain)


eps = 1e-05

def reference(tokens, in_gain, expert_ids, route_weights, gate_weight, up_weight, down_weight, out_gain):
    xf = tokens.astype(jnp.float32)
    normed_in = (xf * lax.rsqrt(lax.optimization_barrier(jnp.mean(xf * xf, axis=1, keepdims=True)) + eps) * in_gain.astype(jnp.float32)).astype(jnp.bfloat16)
    ids = expert_ids.reshape(N_EP, TOK_DEV * TOP_K)
    onehot = (ids[:, :, None] == jnp.arange(EXPERTS, dtype=jnp.int32)[None, None, :]).astype(jnp.int32)
    earlier = jnp.cumsum(onehot, axis=1) - onehot
    slot = lax.optimization_barrier(jnp.sum(earlier * onehot, axis=2))
    block = jnp.arange(N_EP, dtype=jnp.int32)[:, None]
    row_of = ((ids * N_EP + block) * CAP + slot).reshape(-1).astype(jnp.int32)
    token_of = (jnp.arange(TOKENS * TOP_K, dtype=jnp.int32) // TOP_K).astype(jnp.int32)
    row_token = jnp.full((EXPERTS * N_EP * CAP,), TOKENS, jnp.int32).at[row_of].set(token_of)
    row_token = row_token.reshape(EXPERTS, N_EP * CAP)
    extended = jnp.concatenate([normed_in, jnp.zeros((1, D), jnp.bfloat16)], axis=0)

    def expert_rows(args):
        picks, w_gate, w_up, w_down = args
        rows = extended[picks]
        gate_pre = jnp.dot(rows, w_gate, preferred_element_type=jnp.float32)
        up_pre = jnp.dot(rows, w_up, preferred_element_type=jnp.float32)
        g = jnp.minimum(gate_pre, 7.0)
        u = jnp.clip(up_pre, -7.0, 7.0)
        act = (g * jax.nn.sigmoid(1.702 * g) * (u + 1.0)).astype(jnp.bfloat16)
        groups = act.reshape(N_EP * CAP, N_TP, FF // N_TP).astype(jnp.float32)
        wd = w_down.reshape(N_TP, FF // N_TP, D).astype(jnp.float32)
        partial_value = jnp.einsum('rgf,gfd->grd', groups, wd).astype(jnp.bfloat16)
        return lax.optimization_barrier(jnp.sum(partial_value.astype(jnp.float32), axis=0)).astype(jnp.bfloat16)
    expert_out = lax.map(expert_rows, (row_token, gate_weight, up_weight, down_weight))
    expert_out = expert_out.reshape(EXPERTS * N_EP * CAP, D)
    picked = expert_out[row_of].astype(jnp.float32).reshape(TOKENS, TOP_K, D)
    combined = lax.optimization_barrier(jnp.sum(picked * route_weights[:, :, None], axis=1))
    scale = lax.rsqrt(lax.optimization_barrier(jnp.mean(combined * combined, axis=1, keepdims=True)) + eps)
    return (combined * scale * out_gain.astype(jnp.float32)).astype(jnp.bfloat16)
```

```python
import functools

import jax
import jax.numpy as jnp
from jax import lax
from jax.experimental import pallas as pl
from jax.experimental.pallas import tpu as pltpu
from jax.sharding import PartitionSpec as P

eps = 1e-05
MESH = pl.DeviceIdType.MESH
F32 = jnp.float32
BF16 = jnp.bfloat16


def source_order(chips):
    offsets = sorted(range(-(chips // 2) + 1, chips // 2 + 1), key=lambda d: (abs(d), d))
    return [d for d in offsets if d % 2 == 0] + [d for d in offsets[::-1] if d % 2 == 1]


def layer(
    n_ep, n_tp, chunks, stride,
    tokens, in_gain, ids, ids_row, route, w_gate_hbm, w_up_hbm, w_down_hbm, out_gain,
    out,
    tok, w_gate, w_up, w_down, outgoing, rows, part_in, part_out, act, total_out, returned, mix_hi, mix_lo,
    sq_send, sq_recv,
    load_sem, disp_send, disp_recv, ag_send, ag_recv, rs_send, rs_recv, ret_send, ret_recv, sq_ssem, sq_rsem,
):
    tok_count, width = tok.shape
    top = ids.shape[1]
    experts = n_ep
    slots = rows.shape[0] // n_tp // n_ep
    feat = width // n_tp
    row_count = n_ep * slots
    per = n_ep // chunks
    size = per * slots
    half = size // 2
    hops = n_tp // 2
    me_t = lax.axis_index("tp")
    me_e = lax.axis_index("ep")
    chip = me_e // 2
    core = lax.rem(me_e, 2)
    chips = n_ep // 2
    right = lax.rem(me_t + 1, n_tp)
    left = lax.rem(me_t + n_tp - 1, n_tp)
    order = [(d, c) for d in source_order(chips) for c in (0, 1)]

    def at_tp(offset):
        return lax.rem(me_t + offset + 2 * n_tp, n_tp)

    def at_ep(offset, other):
        return lax.rem(chip + offset + 2 * chips, chips) * 2 + lax.rem(core + other, 2)

    def block(j, start, count):
        return rows.at[pl.ds(pl.multiple_of(j * row_count + start, slots), count)]

    loads = [pltpu.make_async_copy(tokens, tok, load_sem.at[0])]
    loads.append(pltpu.make_async_copy(w_gate_hbm, w_gate, load_sem.at[1]))
    loads.append(pltpu.make_async_copy(w_up_hbm, w_up, load_sem.at[2]))
    for j in range(n_tp):
        loads.append(
            pltpu.make_async_copy(
                w_down_hbm.at[:, pl.ds(j * feat, feat)], w_down.at[j], load_sem.at[3 + j]
            )
        )
    for load in loads:
        load.start()

    barrier = pltpu.get_barrier_semaphore()
    for j in range(1, n_ep):
        pl.semaphore_signal(
            barrier, inc=1, device_id={"ep": lax.rem(me_e + j, n_ep)}, device_id_type=MESH
        )
    for j in range(1, n_tp):
        pl.semaphore_signal(barrier, inc=1, device_id={"tp": at_tp(j)}, device_id_type=MESH)

    expert = lax.broadcasted_iota(jnp.int32, (experts, tok_count), 0)
    named = ids_row[0:1, :] == expert
    for k in range(1, top):
        named = named | (ids_row[k : k + 1, :] == expert)
    first = lax.broadcasted_iota(jnp.int32, (tok_count, tok_count), 0)
    second = lax.broadcasted_iota(jnp.int32, (tok_count, tok_count), 1)
    earlier = jnp.dot(
        jnp.where(named, 1.0, 0.0).astype(BF16),
        jnp.where(first < second, 1.0, 0.0).astype(BF16),
        preferred_element_type=F32,
    )
    key = jnp.where(named, earlier, -1.0)
    slot_of = lax.broadcasted_iota(jnp.int32, (slots, tok_count), 0).astype(F32)

    loads[0].wait()
    squares = jnp.zeros((tok_count, 128), F32)
    for j in range(width // 128):
        piece = tok[:, j * 128 : (j + 1) * 128].astype(F32)
        squares = squares + piece * piece
    mean = jnp.sum(squares, axis=1, keepdims=True) / width
    mine = pl.ds(pl.multiple_of(me_t * feat, feat), feat)
    normed = (
        tok[:, mine].astype(F32) * lax.rsqrt(mean + eps) * in_gain[:, mine].astype(F32)
    ).astype(BF16)
    group = max(1, 256 // slots)
    for e in range(0, experts, group):
        pick = jnp.concatenate(
            [
                jnp.where(key[i : i + 1, :] == slot_of, 1.0, 0.0).astype(BF16)
                for i in range(e, min(experts, e + group))
            ],
            axis=0,
        )
        outgoing[e * slots : e * slots + pick.shape[0], :] = jnp.dot(
            pick, normed, preferred_element_type=F32
        ).astype(BF16)

    pl.semaphore_wait(barrier, n_ep - 1 + n_tp - 1)

    for k in range(1, n_ep):
        offset, other = order[k]
        peer = at_ep(-offset, other)
        pltpu.make_async_remote_copy(
            src_ref=outgoing.at[pl.ds(pl.multiple_of(peer * slots, slots), slots)],
            dst_ref=block(me_t, k * slots, slots),
            send_sem=disp_send,
            recv_sem=disp_recv.at[k // per],
            device_id={"ep": peer},
            device_id_type=MESH,
        ).start()
    rows[pl.ds(pl.multiple_of(me_t * row_count, slots), slots), :] = outgoing[
        pl.ds(pl.multiple_of(me_e * slots, slots), slots), :
    ]

    def forward(c, s, way, j, start, count):
        pltpu.make_async_remote_copy(
            src_ref=block(j, start, count),
            dst_ref=block(j, start, count),
            send_sem=ag_send.at[way],
            recv_sem=ag_recv.at[way, c, s],
            device_id={"tp": right if way == 0 else left},
            device_id_type=MESH,
        ).start()

    def wait_for(ref, sem, send=False):
        copy = pltpu.make_async_remote_copy(
            src_ref=ref, dst_ref=ref, send_sem=sem, recv_sem=sem, device_id={"tp": right}, device_id_type=MESH
        )
        if send:
            copy.wait_send()
        else:
            copy.wait_recv()

    def piece_of(s, way, start):
        if s < hops - 1:
            return start, size
        return (start, half) if way == 0 else (start + half, half)

    def gather_step(c, s):
        start = c * size
        if s == 0:
            skip = slots if c == 0 else 0
            wait_for(block(me_t, start + skip, size - skip), disp_recv.at[c])
        for way in (0, 1):
            step = -1 if way == 0 else 1
            j = at_tp(step * s)
            if s > 0:
                wait_for(block(j, *piece_of(s - 1, way, start)), ag_recv.at[way, c, s - 1])
            if s < hops:
                forward(c, s, way, j, *piece_of(s, way, start))
        if s == hops:
            if c == 0:
                for load in loads[1:]:
                    load.wait()
            x = jnp.concatenate(
                [rows[j * row_count + start : j * row_count + start + size, :] for j in range(n_tp)],
                axis=1,
            )
            gate = jnp.minimum(jnp.dot(x, w_gate[...], preferred_element_type=F32), 7.0)
            up = jnp.clip(jnp.dot(x, w_up[...], preferred_element_type=F32), -7.0, 7.0)
            act[start : start + size, :] = (
                gate * jax.nn.sigmoid(1.702 * gate) * (up + 1.0)
            ).astype(BF16)

    def sum_step(c, s):
        start = c * size
        if s == 0:
            own = jnp.dot(act[start : start + size, :], w_down[at_tp(hops)], preferred_element_type=F32)
            part_out[0, c, 0, 0:half, :] = own[0:half, :].astype(BF16)
            part_out[1, c, 0, half:size, :] = own[half:size, :].astype(BF16)
        elif s < hops:
            own = [
                jnp.dot(
                    act[start : start + size, :],
                    w_down[at_tp(hops - s if way == 0 else s - hops)],
                    preferred_element_type=F32,
                )
                for way in (0, 1)
            ]
            for way in (0, 1):
                if s == 1:
                    lo = 0 if way == 0 else half
                    wait_for(part_in.at[way, c, 0, pl.ds(lo, half)], rs_recv.at[way, c, 0])
                    fresh = slice(half, size) if way == 0 else slice(0, half)
                    part_out[way, c, 1, lo : lo + half, :] = (
                        own[way][lo : lo + half, :] + part_in[way, c, 0, lo : lo + half, :].astype(F32)
                    ).astype(BF16)
                    part_out[way, c, 1, fresh, :] = own[way][fresh, :].astype(BF16)
                else:
                    wait_for(part_in.at[way, c, s - 1], rs_recv.at[way, c, s - 1])
                    part_out[way, c, s] = (own[way] + part_in[way, c, s - 1].astype(F32)).astype(BF16)
                send_part(c, s, way)
            return
        if s == 0:
            for way in (0, 1):
                send_part(c, 0, way)
            return
        own = jnp.dot(act[start : start + size, :], w_down[me_t], preferred_element_type=F32)
        for way in (0, 1):
            if hops == 1:
                lo = 0 if way == 0 else half
                wait_for(part_in.at[way, c, 0, pl.ds(lo, half)], rs_recv.at[way, c, 0])
            else:
                wait_for(part_in.at[way, c, s - 1], rs_recv.at[way, c, s - 1])
        if hops == 1:
            arrived = jnp.concatenate(
                [part_in[0, c, 0, 0:half, :], part_in[1, c, 0, half:size, :]], axis=0
            ).astype(F32)
        else:
            arrived = part_in[0, c, s - 1].astype(F32) + part_in[1, c, s - 1].astype(F32)
        total_out[start : start + size, :] = (own + arrived).astype(BF16)
        for k in range(c * per, (c + 1) * per):
            offset, other = order[k]
            home = pl.ds(pl.multiple_of(me_e * slots, slots), slots)
            if k == 0:
                returned[home, :] = total_out[0:slots, :]
                continue
            pltpu.make_async_remote_copy(
                src_ref=total_out.at[pl.ds(k * slots, slots)],
                dst_ref=returned.at[home],
                send_sem=ret_send,
                recv_sem=ret_recv,
                device_id={"ep": at_ep(offset, other)},
                device_id_type=MESH,
            ).start()

    def send_part(c, s, way):
        if s == 0:
            piece = pl.ds(0 if way == 0 else half, half)
            src, dst = part_out.at[way, c, 0, piece], part_in.at[way, c, 0, piece]
        else:
            src, dst = part_out.at[way, c, s], part_in.at[way, c, s]
        pltpu.make_async_remote_copy(
            src_ref=src,
            dst_ref=dst,
            send_sem=rs_send.at[way],
            recv_sem=rs_recv.at[way, c, s],
            device_id={"tp": right if way == 0 else left},
            device_id_type=MESH,
        ).start()

    def prepare_mix():
        lane = lax.broadcasted_iota(jnp.int32, (tok_count, experts), 1)
        hits = [ids[:, k : k + 1] == lane for k in range(top)]
        marks = sum(jnp.where(h, 1.0, 0.0) for h in hits).astype(BF16)
        before = jnp.dot(
            jnp.where(second < first, 1.0, 0.0).astype(BF16), marks, preferred_element_type=F32
        )
        dest = [
            ids[:, k : k + 1].astype(F32) * slots
            + jnp.sum(jnp.where(hits[k], before, 0.0), axis=1, keepdims=True)
            for k in range(top)
        ]
        weight = [route[:, k : k + 1] for k in range(top)]
        weight_hi = [w.astype(BF16).astype(F32) for w in weight]
        weight_lo = [w - h for w, h in zip(weight, weight_hi)]
        wide = min(256, row_count)
        for r in range(0, row_count, wide):
            place = (lax.broadcasted_iota(jnp.int32, (tok_count, wide), 1) + r).astype(F32)
            for ref, values in ((mix_hi, weight_hi), (mix_lo, weight_lo)):
                mixed = jnp.zeros((tok_count, wide), F32)
                for k in range(top):
                    mixed = jnp.where(place == dest[k], values[k], mixed)
                ref[:, r : r + wide] = mixed.astype(BF16)

    for tick in range(stride * (chunks - 1) + 2 * hops + 1):
        for c in range(chunks):
            s = tick - stride * c - hops
            if 0 < s <= hops:
                sum_step(c, s)
        for c in range(chunks):
            s = tick - stride * c
            if 0 <= s <= hops:
                gather_step(c, s)
                if s == hops:
                    sum_step(c, 0)
        if tick == 0:
            prepare_mix()

    wait_for(returned.at[pl.ds(0, row_count - slots)], ret_recv)
    combined = jnp.dot(mix_hi[...], returned[...], preferred_element_type=F32) + jnp.dot(
        mix_lo[...], returned[...], preferred_element_type=F32
    )
    own_sq = jnp.broadcast_to(
        jnp.sum(combined * combined, axis=1, keepdims=True), (tok_count, 128)
    ).T[0:8, :]
    sq_send[...] = own_sq
    for j in range(1, n_tp):
        pltpu.make_async_remote_copy(
            src_ref=sq_send,
            dst_ref=sq_recv.at[me_t],
            send_sem=sq_ssem,
            recv_sem=sq_rsem,
            device_id={"tp": at_tp(j)},
            device_id_type=MESH,
        ).start()
    sq_recv[me_t] = own_sq
    wait_for(sq_recv.at[pl.ds(0, n_tp - 1)], sq_rsem)
    sum_sq = sq_recv[0]
    for j in range(1, n_tp):
        sum_sq = sum_sq + sq_recv[j]
    scale = jnp.broadcast_to(lax.rsqrt(sum_sq[0:1, :] / width + eps), (128, tok_count)).T
    out[...] = (
        combined * jnp.concatenate([scale] * (feat // 128), axis=1) * out_gain[...].astype(F32)
    ).astype(BF16)

    wait_for(outgoing.at[pl.ds(0, row_count - slots)], disp_send, True)
    wait_for(total_out.at[pl.ds(0, row_count - slots)], ret_send, True)
    for way in (0, 1):
        sent = (hops - 1) * row_count + row_count // 2
        wait_for(rows.at[pl.ds(0, sent)], ag_send.at[way], True)
        wait_for(rows.at[pl.ds(0, sent)], rs_send.at[way], True)
    wait_for(sq_recv.at[pl.ds(0, n_tp - 1)], sq_ssem, True)


def on_device(
    tokens, in_gain, expert_ids, route_weights, gate_weight, up_weight, down_weight, out_gain
):
    n_ep = lax.axis_size("ep")
    n_tp = lax.axis_size("tp")
    tok_count, width = tokens.shape
    top = expert_ids.shape[1]
    slots = 2 * tok_count * top // n_ep
    feat = width // n_tp
    hidden = gate_weight.shape[2]
    row_count = n_ep * slots
    chunks = max(2, n_ep // 4)
    size = row_count // chunks
    hops = n_tp // 2
    hbm = pl.BlockSpec(memory_space=pl.ANY)
    vmem = pl.BlockSpec(memory_space=pltpu.VMEM)
    dma = pltpu.SemaphoreType.DMA
    return pl.pallas_call(
        functools.partial(layer, n_ep, n_tp, chunks, 2),
        out_shape=jax.ShapeDtypeStruct((tok_count, feat), BF16),
        in_specs=[hbm, vmem, vmem, vmem, vmem, hbm, hbm, hbm, vmem],
        out_specs=vmem,
        scratch_shapes=[
            pltpu.VMEM((tok_count, width), BF16),
            pltpu.VMEM((width, hidden), BF16),
            pltpu.VMEM((width, hidden), BF16),
            pltpu.VMEM((n_tp, hidden, feat), BF16),
            pltpu.VMEM((row_count, feat), BF16),
            pltpu.VMEM((n_tp * row_count, feat), BF16),
            pltpu.VMEM((2, chunks, hops, size, feat), BF16),
            pltpu.VMEM((2, chunks, hops, size, feat), BF16),
            pltpu.VMEM((row_count, hidden), BF16),
            pltpu.VMEM((row_count, feat), BF16),
            pltpu.VMEM((row_count, feat), BF16),
            pltpu.VMEM((tok_count, row_count), BF16),
            pltpu.VMEM((tok_count, row_count), BF16),
            pltpu.VMEM((8, tok_count), F32),
            pltpu.VMEM((n_tp, 8, tok_count), F32),
            dma((3 + n_tp,)),
            dma,
            dma((chunks,)),
            dma((2,)),
            dma((2, chunks, hops)),
            dma((2,)),
            dma((2, chunks, hops)),
            dma,
            dma,
            dma,
            dma,
        ],
        compiler_params=pltpu.CompilerParams(collective_id=0, has_side_effects=True),
        name="layer",
    )(
        tokens,
        in_gain.reshape(1, width),
        expert_ids,
        expert_ids.T,
        route_weights,
        gate_weight[0],
        up_weight[0],
        down_weight[0],
        out_gain.reshape(1, feat),
    )


def solution(mesh):
    placed = (
        P(("grp", "ep"), None),
        P(),
        P(("grp", "ep"), None),
        P(("grp", "ep"), None),
        P("ep", None, "tp"),
        P("ep", None, "tp"),
        P("ep", "tp", None),
        P("tp"),
    )
    return jax.shard_map(
        on_device, mesh=mesh, in_specs=placed, out_specs=P(("grp", "ep"), "tp"), check_vma=False
    )
```

```python
import functools

import jax
import jax.numpy as jnp
from jax import lax
from jax.experimental import pallas as pl
from jax.experimental.pallas import tpu as pltpu
from jax.sharding import PartitionSpec as P

eps = 1e-05
MESH = pl.DeviceIdType.MESH
F32 = jnp.float32
BF16 = jnp.bfloat16


def notice_plan(n_ep, hops):
    plan, given, tick = {}, 1, 0
    while given < n_ep:
        pace = 2 if tick == 0 else (n_ep + 8) // 10 if tick <= hops else (n_ep + 2) // 5
        plan[tick] = list(range(given, min(n_ep, given + pace)))
        given, tick = given + pace, tick + 1
    return plan


def layer(
    n_ep, n_tp, chunks, stride,
    tokens, in_gain, ids_row, route_row, w_gate_hbm, w_up_hbm, w_down_hbm, out_gain,
    out,
    tok, w_gate, w_up, w_down, outgoing, rows, part_in, part_out, act, total_out, returned, mix_hi, mix_lo,
    sq_send, sq_recv,
    load_sem, up_sem, disp_send, disp_recv, ag_send, ag_recv, rs_send, rs_recv, ret_send, ret_recv, sq_ssem, sq_rsem,
):
    tok_count, width = tok.shape
    top = ids_row.shape[0]
    experts = n_ep
    slots = rows.shape[0] // n_tp // n_ep
    feat = width // n_tp
    row_count = n_ep * slots
    per = n_ep // chunks
    size = per * slots
    half = size // 2
    hops = n_tp // 2
    me_t = lax.axis_index("tp")
    me_e = lax.axis_index("ep")
    link = lax.rem(me_e + n_ep - 1, n_ep)
    right = lax.rem(me_t + 1, n_tp)
    left = lax.rem(me_t + n_tp - 1, n_tp)
    def late_place(at):
        return (chunks - 1 - at * chunks // n_ep) * per + per - 1

    def place_of(source, at):
        index = lax.rem(source + n_ep - 1, n_ep)
        held = late_place(at)
        after = jnp.where(index >= held, index + 1, index)
        return jnp.where(source == 0, held, after)

    def source_at(place):
        held = late_place(me_e)
        return jnp.where(place == held, 0, jnp.where(place > held, place, place + 1))

    def at_tp(offset):
        return lax.rem(me_t + offset + 2 * n_tp, n_tp)

    def block(j, start, count):
        return rows.at[pl.ds(pl.multiple_of(j * row_count + start, slots), count)]

    loads = [pltpu.make_async_copy(tokens, tok, load_sem.at[0])]
    loads.append(pltpu.make_async_copy(w_gate_hbm, w_gate, load_sem.at[1]))
    loads.append(pltpu.make_async_copy(w_up_hbm, w_up, load_sem.at[2]))
    for j in range(n_tp):
        loads.append(
            pltpu.make_async_copy(
                w_down_hbm.at[:, pl.ds(j * feat, feat)], w_down.at[j], load_sem.at[3 + j]
            )
        )
    for load in loads:
        load.start()

    barrier = pltpu.get_barrier_semaphore()
    for j in range(1, n_tp):
        pl.semaphore_signal(barrier, inc=1, device_id={"tp": at_tp(j)}, device_id_type=MESH)

    expert = lax.broadcasted_iota(jnp.int32, (experts, tok_count), 0)
    named = ids_row[0:1, :] == expert
    for k in range(1, top):
        named = named | (ids_row[k : k + 1, :] == expert)
    first = lax.broadcasted_iota(jnp.int32, (tok_count, tok_count), 0)
    second = lax.broadcasted_iota(jnp.int32, (tok_count, tok_count), 1)
    earlier = jnp.dot(
        jnp.where(named, 1.0, 0.0).astype(BF16),
        jnp.where(first < second, 1.0, 0.0).astype(BF16),
        preferred_element_type=F32,
    )
    key = jnp.where(named, earlier, -1.0)
    slot_of = lax.broadcasted_iota(jnp.int32, (slots, tok_count), 0).astype(F32)

    loads[0].wait()
    squares = jnp.zeros((tok_count, 128), F32)
    for j in range(width // 128):
        piece = tok[:, j * 128 : (j + 1) * 128].astype(F32)
        squares = squares + piece * piece
    mean = jnp.sum(squares, axis=1, keepdims=True) / width
    mine = pl.ds(pl.multiple_of(me_t * feat, feat), feat)
    normed = (
        tok[:, mine].astype(F32) * lax.rsqrt(mean + eps) * in_gain[:, mine].astype(F32)
    ).astype(BF16)
    group = max(1, 256 // slots)
    for e in range(0, experts, group):
        pick = jnp.concatenate(
            [
                jnp.where(key[i : i + 1, :] == slot_of, 1.0, 0.0).astype(BF16)
                for i in range(e, min(experts, e + group))
            ],
            axis=0,
        )
        outgoing[e * slots : e * slots + pick.shape[0], :] = jnp.dot(
            pick, normed, preferred_element_type=F32
        ).astype(BF16)

    pl.semaphore_wait(barrier, n_tp - 1 + jnp.minimum(link, 1))

    @pl.when(link < n_ep - 1)
    def _():
        pl.semaphore_signal(
            barrier, inc=1, device_id={"ep": lax.rem(me_e + 1, n_ep)}, device_id_type=MESH
        )

    my_place = place_of(me_e, me_e)

    def dispatch(peer):
        place = place_of(me_e, peer)
        pltpu.make_async_remote_copy(
            src_ref=outgoing.at[pl.ds(pl.multiple_of(peer * slots, slots), slots)],
            dst_ref=block(me_t, place * slots, slots),
            send_sem=disp_send,
            recv_sem=disp_recv.at[place],
            device_id={"ep": peer},
            device_id_type=MESH,
        ).start()

    for d in range(n_ep - 1, 0, -1):

        @pl.when(link >= d)
        def _(d=d):
            peer = lax.rem(me_e - d + n_ep, n_ep)
            pl.semaphore_signal(up_sem.at[d], inc=1, device_id={"ep": peer}, device_id_type=MESH)
            dispatch(peer)

    def notice(d):
        @pl.when(link + d < n_ep)
        def _():
            pl.semaphore_wait(up_sem.at[d], 1)
            dispatch(lax.rem(me_e + d, n_ep))

    rows[pl.ds(pl.multiple_of(me_t * row_count + my_place * slots, slots), slots), :] = outgoing[
        pl.ds(pl.multiple_of(me_e * slots, slots), slots), :
    ]

    def forward(c, s, way, j, start, count):
        pltpu.make_async_remote_copy(
            src_ref=block(j, start, count),
            dst_ref=block(j, start, count),
            send_sem=ag_send.at[way],
            recv_sem=ag_recv.at[way, c, s],
            device_id={"tp": right if way == 0 else left},
            device_id_type=MESH,
        ).start()

    def wait_for(ref, sem, send=False):
        copy = pltpu.make_async_remote_copy(
            src_ref=ref, dst_ref=ref, send_sem=sem, recv_sem=sem, device_id={"tp": right}, device_id_type=MESH
        )
        if send:
            copy.wait_send()
        else:
            copy.wait_recv()

    def piece_of(s, way, start):
        if s < hops - 1:
            return start, size
        return (start, half) if way == 0 else (start + half, half)

    def gather_step(c, s):
        start = c * size
        if s == 0:
            for place in range(c * per, (c + 1) * per):

                @pl.when(my_place != place)
                def _(place=place):
                    wait_for(block(me_t, place * slots, slots), disp_recv.at[place])

        for way in (0, 1):
            step = -1 if way == 0 else 1
            j = at_tp(step * s)
            if s > 0:
                wait_for(block(j, *piece_of(s - 1, way, start)), ag_recv.at[way, c, s - 1])
            if s < hops:
                forward(c, s, way, j, *piece_of(s, way, start))
        if s == hops:
            if c == 0:
                for load in loads[1:]:
                    load.wait()
            x = jnp.concatenate(
                [rows[j * row_count + start : j * row_count + start + size, :] for j in range(n_tp)],
                axis=1,
            )
            gate = jnp.minimum(jnp.dot(x, w_gate[...], preferred_element_type=F32), 7.0)
            up = jnp.clip(jnp.dot(x, w_up[...], preferred_element_type=F32), -7.0, 7.0)
            act[start : start + size, :] = (
                gate * jax.nn.sigmoid(1.702 * gate) * (up + 1.0)
            ).astype(BF16)

    def sum_step(c, s):
        start = c * size
        if s == 0:
            own = jnp.dot(act[start : start + size, :], w_down[at_tp(hops)], preferred_element_type=F32)
            part_out[0, c, 0, 0:half, :] = own[0:half, :].astype(BF16)
            part_out[1, c, 0, half:size, :] = own[half:size, :].astype(BF16)
        elif s < hops:
            own = [
                jnp.dot(
                    act[start : start + size, :],
                    w_down[at_tp(hops - s if way == 0 else s - hops)],
                    preferred_element_type=F32,
                )
                for way in (0, 1)
            ]
            for way in (0, 1):
                if s == 1:
                    lo = 0 if way == 0 else half
                    wait_for(part_in.at[way, c, 0, pl.ds(lo, half)], rs_recv.at[way, c, 0])
                    fresh = slice(half, size) if way == 0 else slice(0, half)
                    part_out[way, c, 1, lo : lo + half, :] = (
                        own[way][lo : lo + half, :] + part_in[way, c, 0, lo : lo + half, :].astype(F32)
                    ).astype(BF16)
                    part_out[way, c, 1, fresh, :] = own[way][fresh, :].astype(BF16)
                else:
                    wait_for(part_in.at[way, c, s - 1], rs_recv.at[way, c, s - 1])
                    part_out[way, c, s] = (own[way] + part_in[way, c, s - 1].astype(F32)).astype(BF16)
                send_part(c, s, way)
            return
        if s == 0:
            for way in (0, 1):
                send_part(c, 0, way)
            return
        own = jnp.dot(act[start : start + size, :], w_down[me_t], preferred_element_type=F32)
        for way in (0, 1):
            if hops == 1:
                lo = 0 if way == 0 else half
                wait_for(part_in.at[way, c, 0, pl.ds(lo, half)], rs_recv.at[way, c, 0])
            else:
                wait_for(part_in.at[way, c, s - 1], rs_recv.at[way, c, s - 1])
        if hops == 1:
            arrived = jnp.concatenate(
                [part_in[0, c, 0, 0:half, :], part_in[1, c, 0, half:size, :]], axis=0
            ).astype(F32)
        else:
            arrived = part_in[0, c, s - 1].astype(F32) + part_in[1, c, s - 1].astype(F32)
        total_out[start : start + size, :] = (own + arrived).astype(BF16)
        home = pl.ds(pl.multiple_of(me_e * slots, slots), slots)
        for place in range(c * per, (c + 1) * per):

            @pl.when(my_place == place)
            def _(place=place):
                returned[home, :] = total_out[place * slots : (place + 1) * slots, :]

            @pl.when(my_place != place)
            def _(place=place):
                pltpu.make_async_remote_copy(
                    src_ref=total_out.at[pl.ds(place * slots, slots)],
                    dst_ref=returned.at[home],
                    send_sem=ret_send,
                    recv_sem=ret_recv,
                    device_id={"ep": source_at(place)},
                    device_id_type=MESH,
                ).start()

    def send_part(c, s, way):
        if s == 0:
            piece = pl.ds(0 if way == 0 else half, half)
            src, dst = part_out.at[way, c, 0, piece], part_in.at[way, c, 0, piece]
        else:
            src, dst = part_out.at[way, c, s], part_in.at[way, c, s]
        pltpu.make_async_remote_copy(
            src_ref=src,
            dst_ref=dst,
            send_sem=rs_send.at[way],
            recv_sem=rs_recv.at[way, c, s],
            device_id={"tp": right if way == 0 else left},
            device_id_type=MESH,
        ).start()

    def prepare_mix():
        def column(row):
            return jnp.broadcast_to(row, (128, tok_count)).T[:, 0:1]

        ids = [column(ids_row[k : k + 1, :].astype(F32)) for k in range(top)]
        lane = lax.broadcasted_iota(jnp.int32, (tok_count, experts), 1).astype(F32)
        hits = [ids[k] == lane for k in range(top)]
        marks = sum(jnp.where(h, 1.0, 0.0) for h in hits).astype(BF16)
        before = jnp.dot(
            jnp.where(second < first, 1.0, 0.0).astype(BF16), marks, preferred_element_type=F32
        )
        dest = [
            ids[k] * slots
            + jnp.sum(jnp.where(hits[k], before, 0.0), axis=1, keepdims=True)
            for k in range(top)
        ]
        weight = [column(route_row[k : k + 1, :]) for k in range(top)]
        weight_hi = [w.astype(BF16).astype(F32) for w in weight]
        weight_lo = [w - h for w, h in zip(weight, weight_hi)]
        wide = min(256, row_count)
        for r in range(0, row_count, wide):
            place = (lax.broadcasted_iota(jnp.int32, (tok_count, wide), 1) + r).astype(F32)
            for ref, values in ((mix_hi, weight_hi), (mix_lo, weight_lo)):
                mixed = jnp.zeros((tok_count, wide), F32)
                for k in range(top):
                    mixed = jnp.where(place == dest[k], values[k], mixed)
                ref[:, r : r + wide] = mixed.astype(BF16)

    plan = notice_plan(n_ep, hops)
    for tick in range(stride * (chunks - 1) + 2 * hops + 1):
        noticed = plan.get(tick, [])
        for d in noticed[: len(noticed) // 2]:
            notice(d)
        for c in range(chunks):
            s = tick - stride * c - hops
            if 0 < s <= hops:
                sum_step(c, s)
        for d in noticed[len(noticed) // 2 :]:
            notice(d)
        for c in range(chunks):
            s = tick - stride * c
            if 0 <= s <= hops:
                gather_step(c, s)
                if s == hops:
                    sum_step(c, 0)
        if tick == 0:
            prepare_mix()

    wait_for(returned.at[pl.ds(0, row_count - slots)], ret_recv)
    combined = jnp.dot(mix_hi[...], returned[...], preferred_element_type=F32) + jnp.dot(
        mix_lo[...], returned[...], preferred_element_type=F32
    )
    own_sq = jnp.broadcast_to(
        jnp.sum(combined * combined, axis=1, keepdims=True), (tok_count, 128)
    ).T[0:8, :]
    sq_send[...] = own_sq
    for j in range(1, n_tp):
        pltpu.make_async_remote_copy(
            src_ref=sq_send,
            dst_ref=sq_recv.at[me_t],
            send_sem=sq_ssem,
            recv_sem=sq_rsem,
            device_id={"tp": at_tp(j)},
            device_id_type=MESH,
        ).start()
    sq_recv[me_t] = own_sq
    wait_for(sq_recv.at[pl.ds(0, n_tp - 1)], sq_rsem)
    sum_sq = sq_recv[0]
    for j in range(1, n_tp):
        sum_sq = sum_sq + sq_recv[j]
    scale = jnp.broadcast_to(lax.rsqrt(sum_sq[0:1, :] / width + eps), (128, tok_count)).T
    out[...] = (
        combined * jnp.concatenate([scale] * (feat // 128), axis=1) * out_gain[...].astype(F32)
    ).astype(BF16)

    wait_for(outgoing.at[pl.ds(0, row_count - slots)], disp_send, True)
    wait_for(total_out.at[pl.ds(0, row_count - slots)], ret_send, True)
    for way in (0, 1):
        sent = (hops - 1) * row_count + row_count // 2
        wait_for(rows.at[pl.ds(0, sent)], ag_send.at[way], True)
        wait_for(rows.at[pl.ds(0, sent)], rs_send.at[way], True)
    wait_for(sq_recv.at[pl.ds(0, n_tp - 1)], sq_ssem, True)


def on_device(
    tokens, in_gain, expert_ids, route_weights, gate_weight, up_weight, down_weight, out_gain
):
    n_ep = lax.axis_size("ep")
    n_tp = lax.axis_size("tp")
    tok_count, width = tokens.shape
    top = expert_ids.shape[1]
    slots = 2 * tok_count * top // n_ep
    feat = width // n_tp
    hidden = gate_weight.shape[2]
    row_count = n_ep * slots
    chunks = max(2, n_ep // 4)
    size = row_count // chunks
    hops = n_tp // 2
    hbm = pl.BlockSpec(memory_space=pl.ANY)
    vmem = pl.BlockSpec(memory_space=pltpu.VMEM)
    dma = pltpu.SemaphoreType.DMA
    return pl.pallas_call(
        functools.partial(layer, n_ep, n_tp, chunks, 1),
        out_shape=jax.ShapeDtypeStruct((tok_count, feat), BF16),
        in_specs=[hbm, vmem, vmem, vmem, hbm, hbm, hbm, vmem],
        out_specs=vmem,
        scratch_shapes=[
            pltpu.VMEM((tok_count, width), BF16),
            pltpu.VMEM((width, hidden), BF16),
            pltpu.VMEM((width, hidden), BF16),
            pltpu.VMEM((n_tp, hidden, feat), BF16),
            pltpu.VMEM((row_count, feat), BF16),
            pltpu.VMEM((n_tp * row_count, feat), BF16),
            pltpu.VMEM((2, chunks, hops, size, feat), BF16),
            pltpu.VMEM((2, chunks, hops, size, feat), BF16),
            pltpu.VMEM((row_count, hidden), BF16),
            pltpu.VMEM((row_count, feat), BF16),
            pltpu.VMEM((row_count, feat), BF16),
            pltpu.VMEM((tok_count, row_count), BF16),
            pltpu.VMEM((tok_count, row_count), BF16),
            pltpu.VMEM((8, tok_count), F32),
            pltpu.VMEM((n_tp, 8, tok_count), F32),
            dma((3 + n_tp,)),
            pltpu.SemaphoreType.REGULAR((n_ep,)),
            dma,
            dma((n_ep,)),
            dma((2,)),
            dma((2, chunks, hops)),
            dma((2,)),
            dma((2, chunks, hops)),
            dma,
            dma,
            dma,
            dma,
        ],
        compiler_params=pltpu.CompilerParams(collective_id=0, has_side_effects=True),
        name="layer",
    )(
        tokens,
        in_gain.reshape(1, width),
        expert_ids.T,
        route_weights.T,
        gate_weight[0],
        up_weight[0],
        down_weight[0],
        out_gain.reshape(1, feat),
    )


def solution(mesh):
    placed = (
        P(("grp", "ep"), None),
        P(),
        P(("grp", "ep"), None),
        P(("grp", "ep"), None),
        P("ep", None, "tp"),
        P("ep", None, "tp"),
        P("ep", "tp", None),
        P("tp"),
    )
    return jax.shard_map(
        on_device, mesh=mesh, in_specs=placed, out_specs=P(("grp", "ep"), "tp"), check_vma=False
    )
```

```python
import functools

import jax
import jax.numpy as jnp
from jax import lax
from jax.experimental import pallas as pl
from jax.experimental.pallas import tpu as pltpu
from jax.sharding import PartitionSpec as P

eps = 1e-05
MESH = pl.DeviceIdType.MESH
F32 = jnp.float32
BF16 = jnp.bfloat16


def schedule(n_ep, chunks, begin, hops):
    last = max(begin) + 2 * hops
    starts = [0.0]
    for tick in range(last):
        busy = sum(0 <= tick - b < 2 * hops for b in begin)
        starts.append(starts[-1] + max(3.5, 1.25 * busy))
    steps = []
    for tick in range(last + 1):
        now = [("sum", c, tick - begin[c] - hops) for c in range(chunks) if 0 < tick - begin[c] - hops <= hops]
        now += [("gather", c, tick - begin[c]) for c in range(chunks) if 0 <= tick - begin[c] <= hops]
        length = starts[tick + 1] - starts[tick] if tick + 1 < len(starts) else 0.0
        steps += [(starts[tick] + length * i / len(now), step) for i, step in enumerate(now)]
    plan, given = [], 1
    for start, step in steps:
        come = []
        while given < n_ep and given * 45.0 / n_ep + 1.5 <= start:
            come.append(given)
            given += 1
        plan.append((come, step))
    plan[-1] = (plan[-1][0] + list(range(given, n_ep)), plan[-1][1])
    return plan


def layer(
    n_ep, n_tp, chunks, stride,
    tokens, in_gain, ids_row, route_row, w_gate_hbm, w_up_hbm, w_down_hbm, out_gain,
    out,
    tok, w_gate, w_up, w_down, outgoing, rows, part_in, part_out, own_part, total_out, returned, mix_hi, mix_lo,
    sq_send, sq_recv,
    load_sem, up_sem, disp_send, disp_recv, ag_send, ag_recv, rs_send, rs_recv, ret_send, ret_recv, sq_ssem, sq_rsem,
):
    tok_count, width = tok.shape
    top = ids_row.shape[0]
    experts = n_ep
    slots = rows.shape[0] // n_tp // n_ep
    feat = width // n_tp
    row_count = n_ep * slots
    per = n_ep // chunks
    size = per * slots
    half = size // 2
    hops = n_tp // 2
    me_t = lax.axis_index("tp")
    me_e = lax.axis_index("ep")
    link = lax.rem(me_e + n_ep - 1, n_ep)
    right = lax.rem(me_t + 1, n_tp)
    left = lax.rem(me_t + n_tp - 1, n_tp)
    def layout(at):
        group = lax.rem(at + n_ep - 1, n_ep) // per
        final = group == chunks - 1
        held = jnp.where(final, 0, jnp.minimum(chunks - 1, chunks - group)) * per + per - 1
        return group * per, jnp.where(final, per - 1, per), held

    def place_of(source, at):
        begin, own, held = layout(at)
        index = source - 1
        rank = jnp.where(index < begin, index + own, jnp.where(index < begin + own, index - begin, index))
        return jnp.where(source == 0, held, jnp.where(rank >= held, rank + 1, rank))

    def source_at(place):
        begin, own, held = layout(me_e)
        rank = jnp.where(place > held, place - 1, place)
        other = jnp.where(rank - own < begin, rank - own, rank)
        return jnp.where(place == held, 0, jnp.where(rank < own, begin + rank, other) + 1)

    def at_tp(offset):
        return lax.rem(me_t + offset + 2 * n_tp, n_tp)

    def block(j, start, count):
        return rows.at[pl.ds(pl.multiple_of(j * row_count + start, slots), count)]

    loads = [pltpu.make_async_copy(tokens, tok, load_sem.at[0])]
    loads.append(pltpu.make_async_copy(w_gate_hbm, w_gate, load_sem.at[1]))
    loads.append(pltpu.make_async_copy(w_up_hbm, w_up, load_sem.at[2]))
    loads.append(pltpu.make_async_copy(w_down_hbm, w_down, load_sem.at[3]))
    for load in loads:
        load.start()

    barrier = pltpu.get_barrier_semaphore()
    for j in range(1, n_tp):
        pl.semaphore_signal(barrier, inc=1, device_id={"tp": at_tp(j)}, device_id_type=MESH)

    expert = lax.broadcasted_iota(jnp.int32, (experts, tok_count), 0)
    named = ids_row[0:1, :] == expert
    for k in range(1, top):
        named = named | (ids_row[k : k + 1, :] == expert)
    first = lax.broadcasted_iota(jnp.int32, (tok_count, tok_count), 0)
    second = lax.broadcasted_iota(jnp.int32, (tok_count, tok_count), 1)
    earlier = jnp.dot(
        jnp.where(named, 1.0, 0.0).astype(BF16),
        jnp.where(first < second, 1.0, 0.0).astype(BF16),
        preferred_element_type=F32,
    )
    key = jnp.where(named, earlier, -1.0)
    slot_of = lax.broadcasted_iota(jnp.int32, (slots, tok_count), 0).astype(F32)

    loads[0].wait()
    squares = jnp.zeros((tok_count, 128), F32)
    for j in range(width // 128):
        piece = tok[:, j * 128 : (j + 1) * 128].astype(F32)
        squares = squares + piece * piece
    mean = jnp.sum(squares, axis=1, keepdims=True) / width
    mine = pl.ds(pl.multiple_of(me_t * feat, feat), feat)
    normed = (
        tok[:, mine].astype(F32) * lax.rsqrt(mean + eps) * in_gain[mine].astype(F32).reshape(1, feat)
    ).astype(BF16)
    group = max(1, 256 // slots)
    for e in range(0, experts, group):
        pick = jnp.concatenate(
            [
                jnp.where(key[i : i + 1, :] == slot_of, 1.0, 0.0).astype(BF16)
                for i in range(e, min(experts, e + group))
            ],
            axis=0,
        )
        outgoing[e * slots : e * slots + pick.shape[0], :] = jnp.dot(
            pick, normed, preferred_element_type=F32
        ).astype(BF16)

    pl.semaphore_wait(barrier, n_tp - 1 + jnp.minimum(link, 1))

    @pl.when(link < n_ep - 1)
    def _():
        pl.semaphore_signal(
            barrier, inc=1, device_id={"ep": lax.rem(me_e + 1, n_ep)}, device_id_type=MESH
        )

    my_place = place_of(me_e, me_e)

    def dispatch(peer):
        place = place_of(me_e, peer)
        pltpu.make_async_remote_copy(
            src_ref=outgoing.at[pl.ds(pl.multiple_of(peer * slots, slots), slots)],
            dst_ref=block(me_t, place * slots, slots),
            send_sem=disp_send,
            recv_sem=disp_recv.at[place],
            device_id={"ep": peer},
            device_id_type=MESH,
        ).start()

    my_group = link // per
    for d in range(1, n_ep):

        @pl.when(link >= d)
        def _(d=d):
            pl.semaphore_signal(
                up_sem.at[d], inc=1, device_id={"ep": lax.rem(me_e - d + n_ep, n_ep)}, device_id_type=MESH
            )

    def send_back(d, due):
        @pl.when(due)
        def _():
            dispatch(lax.rem(me_e - d + n_ep, n_ep))

    for d in range(1, per):
        send_back(d, lax.rem(link, per) >= d)
    def notice(d, due):
        @pl.when(due)
        def _():
            pl.semaphore_wait(up_sem.at[d], 1)
            dispatch(lax.rem(me_e + d, n_ep))

    rows[pl.ds(pl.multiple_of(me_t * row_count + my_place * slots, slots), slots), :] = outgoing[
        pl.ds(pl.multiple_of(me_e * slots, slots), slots), :
    ]

    def forward(c, s, way, j, start, count):
        pltpu.make_async_remote_copy(
            src_ref=block(j, start, count),
            dst_ref=block(j, start, count),
            send_sem=ag_send.at[way],
            recv_sem=ag_recv.at[way, c, s],
            device_id={"tp": right if way == 0 else left},
            device_id_type=MESH,
        ).start()

    def wait_for(ref, sem, send=False):
        copy = pltpu.make_async_remote_copy(
            src_ref=ref, dst_ref=ref, send_sem=sem, recv_sem=sem, device_id={"tp": right}, device_id_type=MESH
        )
        if send:
            copy.wait_send()
        else:
            copy.wait_recv()

    def piece_of(s, way, start):
        if s < hops - 1:
            return start, size
        return (start, half) if way == 0 else (start + half, half)

    def gather_step(c, s):
        start = c * size
        if s == 0:
            for place in range(c * per, (c + 1) * per):

                @pl.when(my_place != place)
                def _(place=place):
                    wait_for(block(me_t, place * slots, slots), disp_recv.at[place])

        for way in (0, 1):
            step = -1 if way == 0 else 1
            j = at_tp(step * s)
            if s > 0:
                wait_for(block(j, *piece_of(s - 1, way, start)), ag_recv.at[way, c, s - 1])
            if s < hops:
                forward(c, s, way, j, *piece_of(s, way, start))
        if s == hops:
            if c == 0:
                for load in loads[1:]:
                    load.wait()
            x = jnp.concatenate(
                [rows[j * row_count + start : j * row_count + start + size, :] for j in range(n_tp)],
                axis=1,
            )
            gate = jnp.minimum(jnp.dot(x, w_gate[...], preferred_element_type=F32), 7.0)
            up = jnp.clip(jnp.dot(x, w_up[...], preferred_element_type=F32), -7.0, 7.0)
            act = (gate * jax.nn.sigmoid(1.702 * gate) * (up + 1.0)).astype(BF16)
            product = jnp.dot(act, w_down[...], preferred_element_type=F32)
            for j in range(n_tp):
                own_part[j, start : start + size, :] = product[:, j * feat : (j + 1) * feat]

    def sum_step(c, s):
        start = c * size
        if s == 0:
            own = own_part[at_tp(hops), start : start + size, :]
            part_out[0, c, 0, 0:half, :] = own[0:half, :].astype(BF16)
            part_out[1, c, 0, half:size, :] = own[half:size, :].astype(BF16)
        elif s < hops:
            own = [
                own_part[at_tp(hops - s if way == 0 else s - hops), start : start + size, :]
                for way in (0, 1)
            ]
            for way in (0, 1):
                if s == 1:
                    lo = 0 if way == 0 else half
                    wait_for(part_in.at[way, c, 0, pl.ds(lo, half)], rs_recv.at[way, c, 0])
                    fresh = slice(half, size) if way == 0 else slice(0, half)
                    part_out[way, c, 1, lo : lo + half, :] = (
                        own[way][lo : lo + half, :] + part_in[way, c, 0, lo : lo + half, :].astype(F32)
                    ).astype(BF16)
                    part_out[way, c, 1, fresh, :] = own[way][fresh, :].astype(BF16)
                else:
                    wait_for(part_in.at[way, c, s - 1], rs_recv.at[way, c, s - 1])
                    part_out[way, c, s] = (own[way] + part_in[way, c, s - 1].astype(F32)).astype(BF16)
                send_part(c, s, way)
            return
        if s == 0:
            for way in (0, 1):
                send_part(c, 0, way)
            return
        own = own_part[me_t, start : start + size, :]
        for way in (0, 1):
            if hops == 1:
                lo = 0 if way == 0 else half
                wait_for(part_in.at[way, c, 0, pl.ds(lo, half)], rs_recv.at[way, c, 0])
            else:
                wait_for(part_in.at[way, c, s - 1], rs_recv.at[way, c, s - 1])
        if hops == 1:
            arrived = jnp.concatenate(
                [part_in[0, c, 0, 0:half, :], part_in[1, c, 0, half:size, :]], axis=0
            ).astype(F32)
        else:
            arrived = part_in[0, c, s - 1].astype(F32) + part_in[1, c, s - 1].astype(F32)
        total_out[start : start + size, :] = (own + arrived).astype(BF16)
        home = pl.ds(pl.multiple_of(me_e * slots, slots), slots)
        for place in range(c * per, (c + 1) * per):

            @pl.when(my_place == place)
            def _(place=place):
                returned[home, :] = total_out[place * slots : (place + 1) * slots, :]

            @pl.when(my_place != place)
            def _(place=place):
                pltpu.make_async_remote_copy(
                    src_ref=total_out.at[pl.ds(place * slots, slots)],
                    dst_ref=returned.at[home],
                    send_sem=ret_send,
                    recv_sem=ret_recv,
                    device_id={"ep": source_at(place)},
                    device_id_type=MESH,
                ).start()

    def send_part(c, s, way):
        if s == 0:
            piece = pl.ds(0 if way == 0 else half, half)
            src, dst = part_out.at[way, c, 0, piece], part_in.at[way, c, 0, piece]
        else:
            src, dst = part_out.at[way, c, s], part_in.at[way, c, s]
        pltpu.make_async_remote_copy(
            src_ref=src,
            dst_ref=dst,
            send_sem=rs_send.at[way],
            recv_sem=rs_recv.at[way, c, s],
            device_id={"tp": right if way == 0 else left},
            device_id_type=MESH,
        ).start()

    def prepare_mix():
        def column(row):
            return jnp.broadcast_to(row, (128, tok_count)).T[:, 0:1]

        ids = [column(ids_row[k : k + 1, :].astype(F32)) for k in range(top)]
        lane = lax.broadcasted_iota(jnp.int32, (tok_count, experts), 1).astype(F32)
        hits = [ids[k] == lane for k in range(top)]
        marks = sum(jnp.where(h, 1.0, 0.0) for h in hits).astype(BF16)
        before = jnp.dot(
            jnp.where(second < first, 1.0, 0.0).astype(BF16), marks, preferred_element_type=F32
        )
        dest = [
            ids[k] * slots
            + jnp.sum(jnp.where(hits[k], before, 0.0), axis=1, keepdims=True)
            for k in range(top)
        ]
        weight = [column(route_row[k : k + 1, :]) for k in range(top)]
        weight_hi = [w.astype(BF16).astype(F32) for w in weight]
        weight_lo = [w - h for w, h in zip(weight, weight_hi)]
        wide = min(256, row_count)
        for r in range(0, row_count, wide):
            place = (lax.broadcasted_iota(jnp.int32, (tok_count, wide), 1) + r).astype(F32)
            for ref, values in ((mix_hi, weight_hi), (mix_lo, weight_lo)):
                mixed = jnp.zeros((tok_count, wide), F32)
                for k in range(top):
                    mixed = jnp.where(place == dest[k], values[k], mixed)
                ref[:, r : r + wide] = mixed.astype(BF16)

    for d in range(1, per):
        notice(d, lax.rem(link, per) + d < per)
    for d in range(n_ep - 1, 0, -1):
        send_back(d, (link >= d) & (lax.rem(link, per) < d))
    def run(begin):
        looked, reached, passed = set(), 0, 0
        for number, (come, (kind, c, s)) in enumerate(schedule(n_ep, chunks, begin, hops)):
            seen = jnp.where(reached > my_group, passed, my_group)
            for d in come:
                looked.add(d)
                notice(d, (link + d < n_ep) & ((link + d) // per > seen))
            if kind == "gather" and s == 0 and c > 0:
                until = min(chunks - 1, c + (1 if c < 3 else 2))
                for d in range(1, min(n_ep, per * (until + 1))):
                    if d not in looked:
                        group = (link + d) // per
                        notice(d, (link + d < n_ep) & (c > my_group) & (group <= until) & (group > seen))
                reached, passed = c, until
            if kind == "sum":
                sum_step(c, s)
            else:
                gather_step(c, s)
                if s == hops:
                    sum_step(c, 0)
            if number == 0:
                prepare_mix()

    early = my_group < chunks // 2

    @pl.when(early)
    def _():
        run([0, 2, 4, 6, 8, 9, 10, 11])

    @pl.when(jnp.logical_not(early))
    def _():
        run(list(range(chunks)))

    wait_for(returned.at[pl.ds(0, row_count - slots)], ret_recv)
    combined = jnp.dot(mix_hi[...], returned[...], preferred_element_type=F32) + jnp.dot(
        mix_lo[...], returned[...], preferred_element_type=F32
    )
    own_sq = jnp.broadcast_to(
        jnp.sum(combined * combined, axis=1, keepdims=True), (tok_count, 128)
    ).T[0:8, :]
    sq_send[...] = own_sq
    for j in range(1, n_tp):
        pltpu.make_async_remote_copy(
            src_ref=sq_send,
            dst_ref=sq_recv.at[me_t],
            send_sem=sq_ssem,
            recv_sem=sq_rsem,
            device_id={"tp": at_tp(j)},
            device_id_type=MESH,
        ).start()
    sq_recv[me_t] = own_sq
    wait_for(sq_recv.at[pl.ds(0, n_tp - 1)], sq_rsem)
    sum_sq = sq_recv[0]
    for j in range(1, n_tp):
        sum_sq = sum_sq + sq_recv[j]
    scale = jnp.broadcast_to(lax.rsqrt(sum_sq[0:1, :] / width + eps), (128, tok_count)).T
    out[...] = (
        combined * jnp.concatenate([scale] * (feat // 128), axis=1) * out_gain[...].astype(F32).reshape(1, feat)
    ).astype(BF16)

    wait_for(outgoing.at[pl.ds(0, row_count - slots)], disp_send, True)
    wait_for(total_out.at[pl.ds(0, row_count - slots)], ret_send, True)
    for way in (0, 1):
        sent = (hops - 1) * row_count + row_count // 2
        wait_for(rows.at[pl.ds(0, sent)], ag_send.at[way], True)
        wait_for(rows.at[pl.ds(0, sent)], rs_send.at[way], True)
    wait_for(sq_recv.at[pl.ds(0, n_tp - 1)], sq_ssem, True)


def on_device(
    tokens, in_gain, expert_ids, route_weights, gate_weight, up_weight, down_weight, out_gain
):
    n_ep = lax.axis_size("ep")
    n_tp = lax.axis_size("tp")
    tok_count, width = tokens.shape
    top = expert_ids.shape[1]
    slots = 2 * tok_count * top // n_ep
    feat = width // n_tp
    hidden = gate_weight.shape[2]
    row_count = n_ep * slots
    chunks = max(2, n_ep // 4)
    size = row_count // chunks
    hops = n_tp // 2
    hbm = pl.BlockSpec(memory_space=pl.ANY)
    vmem = pl.BlockSpec(memory_space=pltpu.VMEM)
    dma = pltpu.SemaphoreType.DMA
    return pl.pallas_call(
        functools.partial(layer, n_ep, n_tp, chunks, 1),
        out_shape=jax.ShapeDtypeStruct((tok_count, feat), BF16),
        in_specs=[hbm, vmem, vmem, vmem, hbm, hbm, hbm, vmem],
        out_specs=vmem,
        scratch_shapes=[
            pltpu.VMEM((tok_count, width), BF16),
            pltpu.VMEM((width, hidden), BF16),
            pltpu.VMEM((width, hidden), BF16),
            pltpu.VMEM((hidden, width), BF16),
            pltpu.VMEM((row_count, feat), BF16),
            pltpu.VMEM((n_tp * row_count, feat), BF16),
            pltpu.VMEM((2, chunks, hops, size, feat), BF16),
            pltpu.VMEM((2, chunks, hops, size, feat), BF16),
            pltpu.VMEM((n_tp, row_count, feat), F32),
            pltpu.VMEM((row_count, feat), BF16),
            pltpu.VMEM((row_count, feat), BF16),
            pltpu.VMEM((tok_count, row_count), BF16),
            pltpu.VMEM((tok_count, row_count), BF16),
            pltpu.VMEM((8, tok_count), F32),
            pltpu.VMEM((n_tp, 8, tok_count), F32),
            dma((4,)),
            pltpu.SemaphoreType.REGULAR((n_ep,)),
            dma,
            dma((n_ep,)),
            dma((2,)),
            dma((2, chunks, hops)),
            dma((2,)),
            dma((2, chunks, hops)),
            dma,
            dma,
            dma,
            dma,
        ],
        compiler_params=pltpu.CompilerParams(collective_id=0, has_side_effects=True),
        name="layer",
    )(
        tokens,
        in_gain,
        expert_ids.T,
        route_weights.T,
        gate_weight[0],
        up_weight[0],
        down_weight[0],
        out_gain,
    )


def solution(mesh):
    placed = (
        P(("grp", "ep"), None),
        P(),
        P(("grp", "ep"), None),
        P(("grp", "ep"), None),
        P("ep", None, "tp"),
        P("ep", None, "tp"),
        P("ep", "tp", None),
        P("tp"),
    )
    return jax.shard_map(
        on_device, mesh=mesh, in_specs=placed, out_specs=P(("grp", "ep"), "tp"), check_vma=False
    )
```

```python
import functools

import jax
import jax.numpy as jnp
from jax import lax
from jax.experimental import pallas as pl
from jax.experimental.pallas import tpu as pltpu
from jax.sharding import PartitionSpec as P

eps = 1e-05
MESH = pl.DeviceIdType.MESH
F32 = jnp.float32
BF16 = jnp.bfloat16


def schedule(n_ep, chunks, begin, hops):
    last = max(begin) + 2 * hops
    starts = [0.0]
    for tick in range(last):
        busy = sum(0 <= tick - b < 2 * hops for b in begin)
        starts.append(starts[-1] + max(3.5, 1.25 * busy))
    steps = []
    for tick in range(last + 1):
        now = [("sum", c, tick - begin[c] - hops) for c in range(chunks) if 0 < tick - begin[c] - hops <= hops]
        now += [("gather", c, tick - begin[c]) for c in range(chunks) if 0 <= tick - begin[c] <= hops]
        length = starts[tick + 1] - starts[tick] if tick + 1 < len(starts) else 0.0
        steps += [(starts[tick] + length * i / len(now), step) for i, step in enumerate(now)]
    plan, given = [], 1
    for start, step in steps:
        come = []
        while given < n_ep and given * 45.0 / n_ep + 1.5 <= start:
            come.append(given)
            given += 1
        plan.append((come, step))
    plan[-1] = (plan[-1][0] + list(range(given, n_ep)), plan[-1][1])
    return plan


def layer(
    n_ep, n_tp, chunks, stride,
    tokens, in_gain, ids_row, route_row, w_gate_hbm, w_up_hbm, w_down_hbm, out_gain,
    out,
    tok, w_gate, w_up, w_down, outgoing, rows, part_in, part_out, own_part, total_out, returned, mix_hi, mix_lo,
    sq_send, sq_recv,
    load_sem, up_sem, disp_send, disp_recv, ag_send, ag_recv, rs_send, rs_recv, ret_send, ret_recv, sq_ssem, sq_rsem,
):
    tok_count, width = tok.shape
    top = ids_row.shape[0]
    experts = n_ep
    slots = rows.shape[0] // n_tp // n_ep
    feat = width // n_tp
    row_count = n_ep * slots
    per = n_ep // chunks
    size = per * slots
    half = size // 2
    hops = n_tp // 2
    me_t = lax.axis_index("tp")
    me_e = lax.axis_index("ep")
    link = lax.rem(me_e + n_ep - 1, n_ep)
    right = lax.rem(me_t + 1, n_tp)
    left = lax.rem(me_t + n_tp - 1, n_tp)
    def layout(at):
        group = lax.rem(at + n_ep - 1, n_ep) // per
        final = group == chunks - 1
        held = jnp.where(final, 0, jnp.minimum(chunks - 1, chunks - group)) * per + per - 1
        return group * per, jnp.where(final, per - 1, per), held

    def place_of(source, at):
        begin, own, held = layout(at)
        index = source - 1
        rank = jnp.where(index < begin, index + own, jnp.where(index < begin + own, index - begin, index))
        return jnp.where(source == 0, held, jnp.where(rank >= held, rank + 1, rank))

    def source_at(place):
        begin, own, held = layout(me_e)
        rank = jnp.where(place > held, place - 1, place)
        other = jnp.where(rank - own < begin, rank - own, rank)
        return jnp.where(place == held, 0, jnp.where(rank < own, begin + rank, other) + 1)

    def at_tp(offset):
        return lax.rem(me_t + offset + 2 * n_tp, n_tp)

    def block(j, start, count):
        return rows.at[pl.ds(pl.multiple_of(j * row_count + start, slots), count)]

    loads = [pltpu.make_async_copy(tokens, tok, load_sem.at[0])]
    loads.append(pltpu.make_async_copy(w_gate_hbm, w_gate, load_sem.at[1]))
    loads.append(pltpu.make_async_copy(w_up_hbm, w_up, load_sem.at[2]))
    loads.append(pltpu.make_async_copy(w_down_hbm, w_down, load_sem.at[3]))
    for load in loads:
        load.start()

    barrier = pltpu.get_barrier_semaphore()
    for j in range(1, n_tp):
        pl.semaphore_signal(barrier, inc=1, device_id={"tp": at_tp(j)}, device_id_type=MESH)

    expert = lax.broadcasted_iota(jnp.int32, (experts, tok_count), 0)
    named = ids_row[0:1, :] == expert
    for k in range(1, top):
        named = named | (ids_row[k : k + 1, :] == expert)
    first = lax.broadcasted_iota(jnp.int32, (tok_count, tok_count), 0)
    second = lax.broadcasted_iota(jnp.int32, (tok_count, tok_count), 1)
    earlier = jnp.dot(
        jnp.where(named, 1.0, 0.0).astype(BF16),
        jnp.where(first < second, 1.0, 0.0).astype(BF16),
        preferred_element_type=F32,
    )
    key = jnp.where(named, earlier, -1.0)
    slot_of = lax.broadcasted_iota(jnp.int32, (slots, tok_count), 0).astype(F32)

    loads[0].wait()
    squares = jnp.zeros((tok_count, 128), F32)
    for j in range(width // 128):
        piece = tok[:, j * 128 : (j + 1) * 128].astype(F32)
        squares = squares + piece * piece
    mean = jnp.sum(squares, axis=1, keepdims=True) / width
    mine = pl.ds(pl.multiple_of(me_t * feat, feat), feat)
    normed = (
        tok[:, mine].astype(F32) * lax.rsqrt(mean + eps) * in_gain[mine].astype(F32).reshape(1, feat)
    ).astype(BF16)
    group = max(1, 256 // slots)
    for e in range(0, experts, group):
        pick = jnp.concatenate(
            [
                jnp.where(key[i : i + 1, :] == slot_of, 1.0, 0.0).astype(BF16)
                for i in range(e, min(experts, e + group))
            ],
            axis=0,
        )
        outgoing[e * slots : e * slots + pick.shape[0], :] = jnp.dot(
            pick, normed, preferred_element_type=F32
        ).astype(BF16)

    pl.semaphore_wait(barrier, n_tp - 1 + jnp.minimum(link, 1))

    @pl.when(link < n_ep - 1)
    def _():
        pl.semaphore_signal(
            barrier, inc=1, device_id={"ep": lax.rem(me_e + 1, n_ep)}, device_id_type=MESH
        )

    my_place = place_of(me_e, me_e)

    def dispatch(peer):
        place = place_of(me_e, peer)
        pltpu.make_async_remote_copy(
            src_ref=outgoing.at[pl.ds(pl.multiple_of(peer * slots, slots), slots)],
            dst_ref=block(me_t, place * slots, slots),
            send_sem=disp_send,
            recv_sem=disp_recv.at[place],
            device_id={"ep": peer},
            device_id_type=MESH,
        ).start()

    my_group = link // per
    for d in range(1, n_ep):

        @pl.when(link >= d)
        def _(d=d):
            pl.semaphore_signal(
                up_sem.at[d], inc=1, device_id={"ep": lax.rem(me_e - d + n_ep, n_ep)}, device_id_type=MESH
            )

    def send_back(d, due):
        @pl.when(due)
        def _():
            dispatch(lax.rem(me_e - d + n_ep, n_ep))

    for d in range(1, per):
        send_back(d, lax.rem(link, per) >= d)
    def notice(d, due):
        @pl.when(due)
        def _():
            pl.semaphore_wait(up_sem.at[d], 1)
            dispatch(lax.rem(me_e + d, n_ep))

    rows[pl.ds(pl.multiple_of(me_t * row_count + my_place * slots, slots), slots), :] = outgoing[
        pl.ds(pl.multiple_of(me_e * slots, slots), slots), :
    ]

    def forward(c, s, way, j, start, count):
        pltpu.make_async_remote_copy(
            src_ref=block(j, start, count),
            dst_ref=block(j, start, count),
            send_sem=ag_send.at[way],
            recv_sem=ag_recv.at[way, c, s],
            device_id={"tp": right if way == 0 else left},
            device_id_type=MESH,
        ).start()

    def wait_for(ref, sem, send=False):
        copy = pltpu.make_async_remote_copy(
            src_ref=ref, dst_ref=ref, send_sem=sem, recv_sem=sem, device_id={"tp": right}, device_id_type=MESH
        )
        if send:
            copy.wait_send()
        else:
            copy.wait_recv()

    def piece_of(s, way, start):
        if s < hops - 1:
            return start, size
        return (start, half) if way == 0 else (start + half, half)

    def gather_step(c, s):
        start = c * size
        if s == 0:
            for place in range(c * per, (c + 1) * per):

                @pl.when(my_place != place)
                def _(place=place):
                    wait_for(block(me_t, place * slots, slots), disp_recv.at[place])

        for way in (0, 1):
            step = -1 if way == 0 else 1
            j = at_tp(step * s)
            if s > 0:
                wait_for(block(j, *piece_of(s - 1, way, start)), ag_recv.at[way, c, s - 1])
            if s < hops:
                forward(c, s, way, j, *piece_of(s, way, start))
        if s == hops:
            if c == 0:
                for load in loads[1:]:
                    load.wait()
            x = jnp.concatenate(
                [rows[j * row_count + start : j * row_count + start + size, :] for j in range(n_tp)],
                axis=1,
            )
            gate = jnp.minimum(jnp.dot(x, w_gate[...], preferred_element_type=F32), 7.0)
            up = jnp.clip(jnp.dot(x, w_up[...], preferred_element_type=F32), -7.0, 7.0)
            act = (gate * jax.nn.sigmoid(1.702 * gate) * (up + 1.0)).astype(BF16)
            product = jnp.dot(act, w_down[...], preferred_element_type=F32)
            for j in range(n_tp):
                own_part[j, start : start + size, :] = product[:, j * feat : (j + 1) * feat]

    def sum_step(c, s):
        start = c * size
        if s == 0:
            own = own_part[at_tp(hops), start : start + size, :]
            part_out[0, c, 0, 0:half, :] = own[0:half, :].astype(BF16)
            part_out[1, c, 0, half:size, :] = own[half:size, :].astype(BF16)
        elif s < hops:
            own = [
                own_part[at_tp(hops - s if way == 0 else s - hops), start : start + size, :]
                for way in (0, 1)
            ]
            for way in (0, 1):
                if s == 1:
                    lo = 0 if way == 0 else half
                    wait_for(part_in.at[way, c, 0, pl.ds(lo, half)], rs_recv.at[way, c, 0])
                    fresh = slice(half, size) if way == 0 else slice(0, half)
                    part_out[way, c, 1, lo : lo + half, :] = (
                        own[way][lo : lo + half, :] + part_in[way, c, 0, lo : lo + half, :].astype(F32)
                    ).astype(BF16)
                    part_out[way, c, 1, fresh, :] = own[way][fresh, :].astype(BF16)
                else:
                    wait_for(part_in.at[way, c, s - 1], rs_recv.at[way, c, s - 1])
                    part_out[way, c, s] = (own[way] + part_in[way, c, s - 1].astype(F32)).astype(BF16)
                send_part(c, s, way)
            return
        if s == 0:
            for way in (0, 1):
                send_part(c, 0, way)
            return
        own = own_part[me_t, start : start + size, :]
        for way in (0, 1):
            if hops == 1:
                lo = 0 if way == 0 else half
                wait_for(part_in.at[way, c, 0, pl.ds(lo, half)], rs_recv.at[way, c, 0])
            else:
                wait_for(part_in.at[way, c, s - 1], rs_recv.at[way, c, s - 1])
        if hops == 1:
            arrived = jnp.concatenate(
                [part_in[0, c, 0, 0:half, :], part_in[1, c, 0, half:size, :]], axis=0
            ).astype(F32)
        else:
            arrived = part_in[0, c, s - 1].astype(F32) + part_in[1, c, s - 1].astype(F32)
        total_out[start : start + size, :] = (own + arrived).astype(BF16)
        home = pl.ds(pl.multiple_of(me_e * slots, slots), slots)
        for place in range(c * per, (c + 1) * per):

            @pl.when(my_place == place)
            def _(place=place):
                returned[home, :] = total_out[place * slots : (place + 1) * slots, :]

            @pl.when(my_place != place)
            def _(place=place):
                pltpu.make_async_remote_copy(
                    src_ref=total_out.at[pl.ds(place * slots, slots)],
                    dst_ref=returned.at[home],
                    send_sem=ret_send,
                    recv_sem=ret_recv,
                    device_id={"ep": source_at(place)},
                    device_id_type=MESH,
                ).start()

    def send_part(c, s, way):
        if s == 0:
            piece = pl.ds(0 if way == 0 else half, half)
            src, dst = part_out.at[way, c, 0, piece], part_in.at[way, c, 0, piece]
        else:
            src, dst = part_out.at[way, c, s], part_in.at[way, c, s]
        pltpu.make_async_remote_copy(
            src_ref=src,
            dst_ref=dst,
            send_sem=rs_send.at[way],
            recv_sem=rs_recv.at[way, c, s],
            device_id={"tp": right if way == 0 else left},
            device_id_type=MESH,
        ).start()

    def prepare_mix():
        def column(row):
            return jnp.broadcast_to(row, (128, tok_count)).T[:, 0:1]

        ids = [column(ids_row[k : k + 1, :].astype(F32)) for k in range(top)]
        lane = lax.broadcasted_iota(jnp.int32, (tok_count, experts), 1).astype(F32)
        hits = [ids[k] == lane for k in range(top)]
        marks = sum(jnp.where(h, 1.0, 0.0) for h in hits).astype(BF16)
        before = jnp.dot(
            jnp.where(second < first, 1.0, 0.0).astype(BF16), marks, preferred_element_type=F32
        )
        dest = [
            ids[k] * slots
            + jnp.sum(jnp.where(hits[k], before, 0.0), axis=1, keepdims=True)
            for k in range(top)
        ]
        weight = [column(route_row[k : k + 1, :]) for k in range(top)]
        weight_hi = [w.astype(BF16).astype(F32) for w in weight]
        weight_lo = [w - h for w, h in zip(weight, weight_hi)]
        wide = min(256, row_count)
        for r in range(0, row_count, wide):
            place = (lax.broadcasted_iota(jnp.int32, (tok_count, wide), 1) + r).astype(F32)
            for ref, values in ((mix_hi, weight_hi), (mix_lo, weight_lo)):
                mixed = jnp.zeros((tok_count, wide), F32)
                for k in range(top):
                    mixed = jnp.where(place == dest[k], values[k], mixed)
                ref[:, r : r + wide] = mixed.astype(BF16)

    for d in range(1, per):
        notice(d, lax.rem(link, per) + d < per)
    for d in range(n_ep - 1, 0, -1):
        send_back(d, (link >= d) & (lax.rem(link, per) < d))
    def run(begin):
        looked, reached, passed = set(), 0, 0
        for number, (come, (kind, c, s)) in enumerate(schedule(n_ep, chunks, begin, hops)):
            seen = jnp.where(reached > my_group, passed, my_group)
            for d in come:
                looked.add(d)
                notice(d, (link + d < n_ep) & ((link + d) // per > seen))
            if kind == "gather" and s == 0 and c > 0:
                until = min(chunks - 1, c + (1 if c < 3 else 2))
                for d in range(1, min(n_ep, per * (until + 1))):
                    if d not in looked:
                        group = (link + d) // per
                        notice(d, (link + d < n_ep) & (c > my_group) & (group <= until) & (group > seen))
                reached, passed = c, until
            if kind == "sum":
                sum_step(c, s)
            else:
                gather_step(c, s)
                if s == hops:
                    sum_step(c, 0)
            if number == 0:
                prepare_mix()

    early = my_group < chunks // 2

    @pl.when(early)
    def _():
        run([0, 2, 4, 6, 8, 9, 10, 11])

    @pl.when(jnp.logical_not(early))
    def _():
        run(list(range(chunks)))

    wait_for(returned.at[pl.ds(0, row_count - slots)], ret_recv)
    combined = jnp.dot(mix_hi[...], returned[...], preferred_element_type=F32) + jnp.dot(
        mix_lo[...], returned[...], preferred_element_type=F32
    )
    own_sq = jnp.broadcast_to(
        jnp.sum(combined * combined, axis=1, keepdims=True), (tok_count, 128)
    ).T[0:8, :]
    sq_send[...] = own_sq
    for j in range(1, n_tp):
        pltpu.make_async_remote_copy(
            src_ref=sq_send,
            dst_ref=sq_recv.at[me_t],
            send_sem=sq_ssem,
            recv_sem=sq_rsem,
            device_id={"tp": at_tp(j)},
            device_id_type=MESH,
        ).start()
    sq_recv[me_t] = own_sq
    wait_for(sq_recv.at[pl.ds(0, n_tp - 1)], sq_rsem)
    sum_sq = sq_recv[0]
    for j in range(1, n_tp):
        sum_sq = sum_sq + sq_recv[j]
    scale = jnp.broadcast_to(lax.rsqrt(sum_sq[0:1, :] / width + eps), (128, tok_count)).T
    out[...] = (
        combined * jnp.concatenate([scale] * (feat // 128), axis=1) * out_gain[...].astype(F32).reshape(1, feat)
    ).astype(BF16)

    wait_for(outgoing.at[pl.ds(0, row_count - slots)], disp_send, True)
    wait_for(total_out.at[pl.ds(0, row_count - slots)], ret_send, True)
    for way in (0, 1):
        sent = (hops - 1) * row_count + row_count // 2
        wait_for(rows.at[pl.ds(0, sent)], ag_send.at[way], True)
        wait_for(rows.at[pl.ds(0, sent)], rs_send.at[way], True)
    wait_for(sq_recv.at[pl.ds(0, n_tp - 1)], sq_ssem, True)


def on_device(
    tokens, in_gain, expert_ids, route_weights, gate_weight, up_weight, down_weight, out_gain
):
    n_ep = lax.axis_size("ep")
    n_tp = lax.axis_size("tp")
    tok_count, width = tokens.shape
    top = expert_ids.shape[1]
    slots = 2 * tok_count * top // n_ep
    feat = width // n_tp
    hidden = gate_weight.shape[2]
    row_count = n_ep * slots
    chunks = max(2, n_ep // 4)
    size = row_count // chunks
    hops = n_tp // 2
    hbm = pl.BlockSpec(memory_space=pl.ANY)
    vmem = pl.BlockSpec(memory_space=pltpu.VMEM)
    dma = pltpu.SemaphoreType.DMA
    return pl.pallas_call(
        functools.partial(layer, n_ep, n_tp, chunks, 1),
        out_shape=pltpu.VMEM((tok_count, feat), BF16),
        in_specs=[hbm, vmem, vmem, vmem, hbm, hbm, hbm, vmem],
        out_specs=vmem,
        scratch_shapes=[
            pltpu.VMEM((tok_count, width), BF16),
            pltpu.VMEM((width, hidden), BF16),
            pltpu.VMEM((width, hidden), BF16),
            pltpu.VMEM((hidden, width), BF16),
            pltpu.VMEM((row_count, feat), BF16),
            pltpu.VMEM((n_tp * row_count, feat), BF16),
            pltpu.VMEM((2, chunks, hops, size, feat), BF16),
            pltpu.VMEM((2, chunks, hops, size, feat), BF16),
            pltpu.VMEM((n_tp, row_count, feat), F32),
            pltpu.VMEM((row_count, feat), BF16),
            pltpu.VMEM((row_count, feat), BF16),
            pltpu.VMEM((tok_count, row_count), BF16),
            pltpu.VMEM((tok_count, row_count), BF16),
            pltpu.VMEM((8, tok_count), F32),
            pltpu.VMEM((n_tp, 8, tok_count), F32),
            dma((4,)),
            pltpu.SemaphoreType.REGULAR((n_ep,)),
            dma,
            dma((n_ep,)),
            dma((2,)),
            dma((2, chunks, hops)),
            dma((2,)),
            dma((2, chunks, hops)),
            dma,
            dma,
            dma,
            dma,
        ],
        compiler_params=pltpu.CompilerParams(collective_id=0, has_side_effects=True),
        name="layer",
    )(
        tokens,
        in_gain,
        expert_ids.T,
        route_weights.T,
        gate_weight[0],
        up_weight[0],
        down_weight[0],
        out_gain,
    )


def solution(mesh):
    placed = (
        P(("grp", "ep"), None),
        P(),
        P(("grp", "ep"), None),
        P(("grp", "ep"), None),
        P("ep", None, "tp"),
        P("ep", None, "tp"),
        P("ep", "tp", None),
        P("tp"),
    )
    return jax.shard_map(
        on_device, mesh=mesh, in_specs=placed, out_specs=P(("grp", "ep"), "tp"), check_vma=False
    )
```
